32 devices in a mesh: fs: 8 (over z, x), tp: 4 (over y, core).
Axes of the slice: x: 2, y: 2, z: 4, core: 2. Of those that a mesh axis runs over, the one named last changes fastest.
Arguments:
- tokens: bfloat16 [2048, 2048], P('fs', 'tp'), may hold values from -6 to 6
- grad_out: bfloat16 [2048, 2048], P('fs', 'tp'), may hold values from -6 to 6
- up_weight: bfloat16 [2048, 4096], P('fs', 'tp'), may hold values from -0.125 to 0.125
- down_weight: bfloat16 [4096, 2048], P('tp', 'fs'), may hold values from -0.09375 to 0.09375
Outputs:
- input_grad: bfloat16 [2048, 2048], P('fs', 'tp')
- up_grad: float32 [2048, 4096], P('fs', 'tp')
- down_grad: float32 [4096, 2048], P('tp', 'fs')
- up_norms: float32 [2048], P('fs')
- down_norms: float32 [4096], P('tp')
The draws below stay inside these ranges and needn't reach their ends.
All inputs are finite; a program needn't handle non-finite values.
Results may differ from the reference program's by a relative error of at most 0.015.
Values may be sent and summed in bfloat16 or wider, within the bound.
A program may use at most 64 MiB of HBM per device.

```python
import jax
import jax.numpy as jnp

D = 2048
FF = 4096
TOKENS = 2048
N_TP = 4


def with_spikes(entries, own_key, source, target, blocks, factor):
    owner, partner = [(jnp.arange(entries.shape[dim]) // (entries.shape[dim] // blocks)).reshape([-1 if axis == dim else 1 for axis in range(entries.ndim)]) for dim in (source, target)]
    chosen = jax.random.permutation(own_key, blocks)[partner]
    strong = (owner == chosen) | (owner == (partner + blocks // 2) % blocks)
    return jnp.where(strong, factor * entries, entries)


def steps_of(key, shape, cuts, low, largest):
    gain = 1.0
    for axis_at, parts in cuts:
        steps = jax.random.uniform(jax.random.fold_in(jax.random.fold_in(key, 6), axis_at), (parts,), jnp.float32, low / len(cuts), largest / len(cuts))
        gain = gain * jnp.repeat(jnp.exp(steps), shape[axis_at] // parts).reshape((-1,) + (1,) * (len(shape) - 1 - axis_at))
    return gain


def centred(rng, shape, spread, bound, split=(), kind=jnp.bfloat16):
    entries = jax.random.normal(rng, shape, jnp.float32) * spread
    if len(split) > 0:
        entries = steps_of(rng, shape, split, -0.22, 0.18) * entries
    return jnp.clip(entries, min=-bound, max=bound).astype(kind)


def heavy_noise(stream_key, dims, spread, reach, shards, heavy, held_as=jnp.bfloat16):
    entries = spread * jax.random.normal(stream_key, dims, jnp.float32)
    if shards:
        entries = entries * steps_of(stream_key, dims, shards, -0.22, 0.18)
    return jnp.clip(with_spikes(entries, jax.random.fold_in(stream_key, 3), *heavy), -reach, reach).astype(held_as)


def setup_inputs(seed: int = 0) -> dict:
    splits = jax.random.split(jax.random.key(seed), 5)
    tokens = heavy_noise(splits[0], (TOKENS, D), 1.0, 6.0, ((0, 8), (1, 4)), (0, 1, 8, 2.0))
    grad_out = heavy_noise(splits[1], (TOKENS, D), 1.0, 6.0, ((0, 8), (1, 4)), (0, 1, 8, 2.0))
    up_weight = centred(splits[2], (D, FF), D ** -0.5, 0.125, ((0, 8), (1, 4)))
    down_weight = centred(splits[3], (FF, D), FF ** -0.5, 0.09375, ((0, 4), (1, 8)))
    return dict(tokens=tokens, grad_out=grad_out, up_weight=up_weight, down_weight=down_weight)


def reference(tokens, grad_out, up_weight, down_weight):
    pre = jnp.dot(tokens, up_weight, preferred_element_type=jnp.float32)
    relued = jnp.maximum(pre, 0.0)
    act = (relued * relued).astype(jnp.bfloat16)
    dact = jnp.dot(grad_out, down_weight.T, preferred_element_type=jnp.float32)
    dpre = (dact * 2.0 * relued).astype(jnp.bfloat16)
    down_grad = jnp.dot(act.T, grad_out, preferred_element_type=jnp.float32)
    up_grad = jnp.dot(tokens.T, dpre, preferred_element_type=jnp.float32)
    block = FF // N_TP
    total = jnp.zeros((tokens.shape[0], D), jnp.float32)
    for index in range(N_TP):
        part = jnp.dot(dpre[:, index * block:(index + 1) * block], up_weight[:, index * block:(index + 1) * block].T, preferred_element_type=jnp.float32)
        total = total + part.astype(jnp.bfloat16).astype(jnp.float32)
    input_grad = total.astype(jnp.bfloat16)
    up_norms = jnp.sum(up_grad * up_grad, axis=1)
    down_norms = jnp.sum(down_grad * down_grad, axis=1)
    return input_grad, up_grad, down_grad, up_norms, down_norms
```

```python
import functools

import jax
import jax.numpy as jnp
from jax import lax
from jax.experimental import pallas as pl
from jax.experimental.pallas import tpu as pltpu
from jax.sharding import PartitionSpec as P

BF = jnp.bfloat16
F32 = jnp.float32


def on_device(tokens, grad_out, up_weight, down_weight):
    rows, cotan = (
        lax.all_gather(tokens, "tp", axis=1, tiled=True),
        lax.all_gather(grad_out, "tp", axis=1, tiled=True),
    )
    up_local = lax.all_gather(up_weight, "fs", axis=0, tiled=True)
    dact = lax.dot_general(
        cotan,
        lax.all_gather(down_weight, "fs", axis=1, tiled=True),
        (((1,), (1,)), ((), ())),
        preferred_element_type=F32,
    )
    pre = jnp.dot(rows, up_local, preferred_element_type=F32)
    relued = jnp.maximum(pre, 0.0)
    act = (relued * relued).astype(BF)
    dpre = (dact * 2.0 * relued).astype(BF)
    partial_sum = lax.dot_general(
        dpre, up_local, (((1,), (1,)), ((), ())), preferred_element_type=F32
    )
    rounded = lax.optimization_barrier(partial_sum.astype(BF))
    input_grad = lax.psum_scatter(rounded, "tp", scatter_dimension=1, tiled=True)
    up_shard = lax.psum_scatter(
        lax.dot_general(
            rows, dpre, (((0,), (0,)), ((), ())), preferred_element_type=F32
        ).astype(BF),
        "fs",
        scatter_dimension=0,
        tiled=True,
    ).astype(F32)
    down_flip = lax.psum_scatter(
        lax.dot_general(
            cotan, act, (((0,), (0,)), ((), ())), preferred_element_type=F32
        ).astype(BF),
        "fs",
        scatter_dimension=0,
        tiled=True,
    ).astype(F32)
    down_grad = down_flip.T
    up_norms = lax.psum(jnp.sum(up_shard * up_shard, axis=1), "tp")
    down_norms = lax.psum(jnp.sum(down_grad * down_grad, axis=1), "fs")
    return (input_grad, up_shard, down_grad, up_norms, down_norms)


def dot(a, b, ca, cb, **kw):
    return lax.dot_general(a, b, (((ca,), (cb,)), ((), ())), preferred_element_type=F32, **kw)


def kernel(Z, tok, grd, upw, dnw, ig_o, ug_o, dg_o, un_o, dn_o,
           TG, UW, DW, ACT, DP, PO, PCs, PCr, PYs, PYr, PZs, PZr,
           GXs, GXr, GZs, GZr, NUs, NUr, NDs, NDr,
           ss, ls, wz, wx, tz, ty, tc, pc, py, pz, gx, gz, nu, nd):
    X = Y = C = 2
    TB, KB = tok.shape
    RB = upw.shape[0]
    HB = upw.shape[1] // Z
    FS, TP = Z * X, Y * C
    f = lax.axis_index("fs")
    t = lax.axis_index("tp")
    z, x = f // X, f % X
    y, c = t // C, t % C
    xn, yn, cn = 1 - x, 1 - y, 1 - c
    DX = {"fs": z * X + xn, "tp": t}
    DY = {"fs": f, "tp": yn * C + c}
    DC = {"fs": f, "tp": y * C + cn}

    def at_z(zz):
        return {"fs": zz * X + x, "tp": t}

    order = []
    for i in range(Z):
        o = jnp.int32(0)
        for zz in range(Z):
            near = sorted(range(Z), key=lambda q: (abs(q - zz), q))
            o = jnp.where(z == zz, near[i], o)
        order.append(o)

    def blk(i, n):
        return pl.ds(pl.multiple_of(i * n, n), n)

    sends = []

    def send(src, dst, rsem, dev, cond=None):
        d = pltpu.make_async_remote_copy(
            src_ref=src, dst_ref=dst, send_sem=ss.at[len(sends)], recv_sem=rsem,
            device_id=dev, device_id_type=pl.DeviceIdType.MESH)
        sends.append((d, cond))
        if cond is None:
            d.start()
        else:
            pl.when(cond)(d.start)

    def got(dst, rsem):
        pltpu.make_async_remote_copy(
            src_ref=dst, dst_ref=dst, send_sem=ss.at[0], recv_sem=rsem,
            device_id=DX, device_id_type=pl.DeviceIdType.MESH).wait_recv()

    bar = pltpu.get_barrier_semaphore()
    for p in range(1, FS):
        pl.semaphore_signal(bar, inc=1, device_id={"fs": (f + p) % FS, "tp": t},
                            device_id_type=pl.DeviceIdType.MESH)
    for p in range(1, TP):
        pl.semaphore_signal(bar, inc=1, device_id={"fs": f, "tp": (t + p) % TP},
                            device_id_type=pl.DeviceIdType.MESH)

    TK = (tok, grd)

    def tgr(a, o, k):
        return TG.at[a, blk(o, TB), blk(k, KB)]

    def w_src(a, zz):
        return upw.at[:, blk(zz, HB)] if a == 0 else dnw.at[blk(zz, HB), :]

    def w_dst(a, ff):
        return UW.at[blk(ff, RB), :] if a == 0 else DW.at[:, blk(ff, RB)]

    local = []
    for a in range(2):
        local.append(pltpu.make_async_copy(w_src(a, z), w_dst(a, f), ls.at[a]))
        local.append(pltpu.make_async_copy(TK[a], tgr(a, z, t), ls.at[2 + a]))
    for d in local:
        d.start()
    pl.semaphore_wait(bar, FS - 1 + TP - 1)

    for a in range(2):
        send(w_src(a, z), w_dst(a, f), wx.at[a, z], DX)
        send(TK[a], tgr(a, z, t), ty.at[a, z], DY)
        send(TK[a], tgr(a, z, t), tc.at[a, z, y], DC)
    for i in range(1, Z):
        for a in range(2):
            send(w_src(a, order[i]), w_dst(a, f), wz.at[a, z], at_z(order[i]))
    up_z = jnp.minimum(z + 1, Z - 1)
    dn_z = jnp.maximum(z - 1, 0)
    for a in range(2):
        send(TK[a], tgr(a, z, t), tz.at[a, z], at_z(up_z), z < Z - 1)
        send(TK[a], tgr(a, z, t), tz.at[a, z], at_z(dn_z), z > 0)

    def arrive(i):
        o = order[i]
        for a in range(2):
            r = tgr(a, o, t)
            got(r, tz.at[a, o])
            send(r, r, tz.at[a, o], at_z(up_z), (o < z) & (z < Z - 1))
            send(r, r, tz.at[a, o], at_z(dn_z), (o > z) & (z > 0))
            send(r, r, ty.at[a, o], DY)
            send(r, r, tc.at[a, o, y], DC)

    def yfwd(i):
        o = order[i]
        for a in range(2):
            r = tgr(a, o, yn * C + c)
            got(r, ty.at[a, o])
            send(r, r, tc.at[a, o, yn], DC)

    def ready(i):
        o = order[i]
        for a in range(2):
            for yy in range(Y):
                got(tgr(a, o, yy * C + cn), tc.at[a, o, yy])

    def hidden(i):
        r = blk(order[i], TB)
        pre = dot(TG[0, r, :], UW[...], 1, 0)
        dact = dot(TG[1, r, :], DW[...], 1, 1)
        relued = jnp.maximum(pre, 0.0)
        ACT[r, :] = (relued * relued).astype(BF)
        DP[r, :] = (dact * 2.0 * relued).astype(BF)

    def back(i):
        d = DP[blk(order[i], TB), :]
        for yy in range(Y):
            for cc, keep in ((cn, False), (c, True)):
                part = dot(d, UW[blk(yy * C + cc, KB), :], 1, 1)
                if keep:
                    PO[i, yy] = part.astype(BF)
                else:
                    PCs[i, yy] = part.astype(BF)
                    send(PCs.at[i, yy], PCr.at[i, yy], pc.at[i, yy], DC)

    def core_sum(i):
        for yy in range(Y):
            got(PCr.at[i, yy], pc.at[i, yy])
        PYs[i] = (PO[i, yn].astype(F32) + PCr[i, yn].astype(F32)).astype(BF)
        send(PYs.at[i], PYr.at[i], py.at[i], DY)

    def y_sum(i):
        got(PYr.at[i], py.at[i])
        s = PO[i, y].astype(F32) + PCr[i, y].astype(F32) + PYr[i].astype(F32)
        if i == 0:
            return s
        PZs[i] = s.astype(BF)
        send(PZs.at[i], PZr.at[z], pz.at[z], at_z(order[i]))

    def grads(a, ff):
        if a == 0:
            return dot(TG[0, :, blk(ff, RB)], DP[...], 0, 0)
        return dot(ACT[...], TG[1, :, blk(ff, RB)], 0, 0)

    for i in range(1, Z):
        o = order[i]
        for a in range(2):
            r = w_dst(a, o * X + x)
            got(r, wz.at[a, o])
            send(r, r, wx.at[a, o], DX)
    yfwd(0)
    arrive(1)
    for d in local:
        d.wait()
    for i in range(Z):
        for a in range(2):
            got(w_dst(a, order[i] * X + xn), wx.at[a, order[i]])
    for i in range(Z):
        ready(i)
        hidden(i)
        if i + 1 < Z:
            back(i)
            yfwd(i + 1)
        if i + 2 < Z:
            arrive(i + 2)
        if i >= 1:
            core_sum(i - 1)
        if i >= 2 and i + 1 < Z:
            y_sum(i - 1)

    far = list(range(Z - 1, -1, -1))
    for i in far:
        for a in range(2):
            GXs[a, i] = grads(a, order[i] * X + xn).astype(BF)
            send(GXs.at[a, i], GXr.at[a, i], gx.at[a, i], DX)
    back(Z - 1)
    if Z > 2:
        y_sum(Z - 2)
    for i in far:
        o = order[i]
        for a in range(2):
            g = grads(a, o * X + x)
            got(GXr.at[a, i], gx.at[a, i])
            g = g + GXr[a, i].astype(F32)
            if i:
                GZs[a, i] = g.astype(BF)
                send(GZs.at[a, i], GZr.at[a, z], gz.at[a, z], at_z(o))
            elif a == 0:
                ug_o[:, blk(o, HB)] = g
            else:
                dg_o[blk(o, HB), :] = g
        if i == Z - 1:
            core_sum(Z - 1)
    y_sum(Z - 1)
    total = y_sum(0)
    for i in range(1, Z):
        got(PZr.at[order[i]], pz.at[order[i]])
        total = total + PZr[order[i]].astype(F32)
    ig_o[...] = total.astype(BF)

    for i in range(1, Z):
        o = order[i]
        for a in range(2):
            got(GZr.at[a, o], gz.at[a, o])
        ug_o[:, blk(o, HB)] = GZr[0, o].astype(F32)
        dg_o[blk(o, HB), :] = GZr[1, o].astype(F32)

    hi = dict(precision=lax.Precision.HIGHEST)
    g = ug_o[...]
    nu_mine = dot(jnp.ones((8, g.shape[1]), F32), g * g, 1, 1, **hi)
    NUs[...] = nu_mine
    for p in range(1, TP):
        send(NUs, NUr.at[t], nu.at[t], {"fs": f, "tp": (t + p) % TP})
    g = dg_o[...]
    nd_mine = dot(jnp.ones((8, g.shape[1]), F32), g * g, 1, 1, **hi)
    NDs[...] = nd_mine
    for p in range(1, FS):
        send(NDs, NDr.at[f], nd.at[f], {"fs": (f + p) % FS, "tp": t})
    NUr[t] = nu_mine
    NDr[f] = nd_mine
    for p in range(1, TP):
        q = (t + p) % TP
        got(NUr.at[q], nu.at[q])
    for p in range(1, FS):
        q = (f + p) % FS
        got(NDr.at[q], nd.at[q])
    un_o[...] = sum(NUr[q] for q in range(TP))
    dn_o[...] = sum(NDr[q] for q in range(FS))

    for d, cond in sends:
        if cond is None:
            d.wait_send()
        else:
            pl.when(cond)(d.wait_send)


def fused(Z, tokens, grad_out, up_weight, down_weight):
    TB, KB = tokens.shape
    RB, HL = up_weight.shape
    HB, X, Y, C = HL // Z, 2, 2, 2
    FS, TP = Z * X, Y * C
    D, T = KB * TP, TB * Z
    V, S = pltpu.VMEM, pltpu.SemaphoreType.DMA
    any_ = pl.BlockSpec(memory_space=pl.ANY)
    vm = pl.BlockSpec(memory_space=pltpu.VMEM)
    n_sends = 2 * 3 + 2 * (Z - 1) + 4 + 8 * (Z - 1) + 2 * Z + 2 * (Z - 1)
    n_sends += 2 * Z + Z + Z - 1 + 2 * Z + 2 * (Z - 1) + TP - 1 + FS - 1
    outs = pl.pallas_call(
        functools.partial(kernel, Z),
        out_shape=(
            jax.ShapeDtypeStruct((TB, KB), BF),
            jax.ShapeDtypeStruct((RB, HL), F32),
            jax.ShapeDtypeStruct((HL, RB), F32),
            jax.ShapeDtypeStruct((8, RB), F32),
            jax.ShapeDtypeStruct((8, HL), F32),
        ),
        in_specs=[any_] * 4,
        out_specs=[vm] * 5,
        scratch_shapes=[
            V((2, T, D), BF), V((D, HB), BF), V((HB, D), BF), V((T, HB), BF), V((T, HB), BF),
            V((Z, Y, TB, KB), BF), V((Z, Y, TB, KB), BF), V((Z, Y, TB, KB), BF),
            V((Z, TB, KB), BF), V((Z, TB, KB), BF), V((Z, TB, KB), BF), V((Z, TB, KB), BF),
            V((2, Z, RB, HB), BF), V((2, Z, RB, HB), BF), V((2, Z, RB, HB), BF), V((2, Z, RB, HB), BF),
            V((8, RB), F32), V((TP, 8, RB), F32), V((8, HL), F32), V((FS, 8, HL), F32),
            S((n_sends,)), S((4,)), S((2, Z)), S((2, Z)), S((2, Z)), S((2, Z)), S((2, Z, Y)),
            S((Z, Y)), S((Z,)), S((Z,)), S((2, Z)), S((2, Z)), S((TP,)), S((FS,)),
        ],
        compiler_params=pltpu.CompilerParams(
            collective_id=0, has_side_effects=True, vmem_limit_bytes=60 * 1024 * 1024
        ),
        name="ffn_bwd",
    )(tokens, grad_out, up_weight, down_weight)
    ig, ug, dg, un, dn = outs
    return ig, ug, dg, un[0], dn[0]


def solution(mesh):
    fs, tp = mesh.shape["fs"], mesh.shape["tp"]
    xs = tp // 2
    zs = fs // xs

    def body(tokens, grad_out, up_weight, down_weight):
        pairs = xs == 2 and tp == 4 and zs >= 2 and up_weight.shape[1] % (128 * zs) == 0
        fits = tokens.shape[0] * zs * tokens.shape[1] * tp * 4 <= 16 * 2**20
        square = up_weight.shape[0] == up_weight.shape[1] // zs
        if pairs and fits and square:
            return fused(zs, tokens, grad_out, up_weight, down_weight)
        return on_device(tokens, grad_out, up_weight, down_weight)

    return jax.shard_map(
        body,
        mesh=mesh,
        in_specs=(P("fs", "tp"), P("fs", "tp"), P("fs", "tp"), P("tp", "fs")),
        out_specs=(P("fs", "tp"), P("fs", "tp"), P("tp", "fs"), P("fs"), P("tp")),
        check_vma=False,
    )
```

```python
import functools

import jax
import jax.numpy as jnp
from jax import lax
from jax.experimental import pallas as pl
from jax.experimental.pallas import tpu as pltpu
from jax.sharding import PartitionSpec as P

BF = jnp.bfloat16
F32 = jnp.float32


def on_device(tokens, grad_out, up_weight, down_weight):
    rows, cotan = (
        lax.all_gather(tokens, "tp", axis=1, tiled=True),
        lax.all_gather(grad_out, "tp", axis=1, tiled=True),
    )
    up_local = lax.all_gather(up_weight, "fs", axis=0, tiled=True)
    dact = lax.dot_general(
        cotan,
        lax.all_gather(down_weight, "fs", axis=1, tiled=True),
        (((1,), (1,)), ((), ())),
        preferred_element_type=F32,
    )
    pre = jnp.dot(rows, up_local, preferred_element_type=F32)
    relued = jnp.maximum(pre, 0.0)
    act = (relued * relued).astype(BF)
    dpre = (dact * 2.0 * relued).astype(BF)
    partial_sum = lax.dot_general(
        dpre, up_local, (((1,), (1,)), ((), ())), preferred_element_type=F32
    )
    rounded = lax.optimization_barrier(partial_sum.astype(BF))
    input_grad = lax.psum_scatter(rounded, "tp", scatter_dimension=1, tiled=True)
    up_shard = lax.psum_scatter(
        lax.dot_general(
            rows, dpre, (((0,), (0,)), ((), ())), preferred_element_type=F32
        ).astype(BF),
        "fs",
        scatter_dimension=0,
        tiled=True,
    ).astype(F32)
    down_flip = lax.psum_scatter(
        lax.dot_general(
            cotan, act, (((0,), (0,)), ((), ())), preferred_element_type=F32
        ).astype(BF),
        "fs",
        scatter_dimension=0,
        tiled=True,
    ).astype(F32)
    down_grad = down_flip.T
    up_norms = lax.psum(jnp.sum(up_shard * up_shard, axis=1), "tp")
    down_norms = lax.psum(jnp.sum(down_grad * down_grad, axis=1), "fs")
    return (input_grad, up_shard, down_grad, up_norms, down_norms)


def dot(a, b, ca, cb, **kw):
    return lax.dot_general(a, b, (((ca,), (cb,)), ((), ())), preferred_element_type=F32, **kw)


def kernel(Z, H, tok, grd, upw, dnw, ig_o, ug_o, dg_o, un_o, dn_o,
           TG, UW, DW, ACT, DP, PO, PCs, PCr, PYs, PYr, PZs, PZr, PZd,
           ACC, GXs, GXr, GZs, GZr, NUs, NUr, NDs, NDr,
           ss, ls, wz, wx, tz, ty, tc, pc, py, pz, pd, gx, gz, nu, nd):
    X = Y = C = 2
    TB, KB = tok.shape
    RB = upw.shape[0]
    HB = upw.shape[1] // Z
    FS, TP = Z * X, Y * C
    f = lax.axis_index("fs")
    t = lax.axis_index("tp")
    z, x = f // X, f % X
    y, c = t // C, t % C
    xn, yn, cn = 1 - x, 1 - y, 1 - c
    DX = {"fs": z * X + xn, "tp": t}
    DY = {"fs": f, "tp": yn * C + c}
    DC = {"fs": f, "tp": y * C + cn}

    def at_z(zz):
        return {"fs": zz * X + x, "tp": t}

    order = []
    for i in range(Z):
        o = jnp.int32(0)
        for zz in range(Z):
            near = sorted(range(Z), key=lambda q: (abs(q - zz), q))
            o = jnp.where(z == zz, near[i], o)
        order.append(o)

    def blk(i, n):
        return pl.ds(pl.multiple_of(i * n, n), n)

    sends = []

    def send(src, dst, rsem, dev, cond=None):
        d = pltpu.make_async_remote_copy(
            src_ref=src, dst_ref=dst, send_sem=ss.at[len(sends)], recv_sem=rsem,
            device_id=dev, device_id_type=pl.DeviceIdType.MESH)
        sends.append((d, cond))
        if cond is None:
            d.start()
        else:
            pl.when(cond)(d.start)

    def got(dst, rsem):
        pltpu.make_async_remote_copy(
            src_ref=dst, dst_ref=dst, send_sem=ss.at[0], recv_sem=rsem,
            device_id=DX, device_id_type=pl.DeviceIdType.MESH).wait_recv()

    bar = pltpu.get_barrier_semaphore()
    for p in range(1, FS):
        pl.semaphore_signal(bar, inc=1, device_id={"fs": (f + p) % FS, "tp": t},
                            device_id_type=pl.DeviceIdType.MESH)
    for p in range(1, TP):
        pl.semaphore_signal(bar, inc=1, device_id={"fs": f, "tp": (t + p) % TP},
                            device_id_type=pl.DeviceIdType.MESH)

    TK = (tok, grd)

    TS = TB // H
    pieces = [(a, h) for a in range(2) for h in range(H)]

    def tgr(a, o, k, h):
        return TG.at[a, blk(o * H + h, TS), blk(k, KB)]

    def mine(a, h):
        return TK[a].at[pl.ds(h * TS, TS), :]

    def w_src(a, zz):
        return upw.at[:, blk(zz, HB)] if a == 0 else dnw.at[blk(zz, HB), :]

    def w_dst(a, ff):
        return UW.at[blk(ff, RB), :] if a == 0 else DW.at[:, blk(ff, RB)]

    local = []
    for a in range(2):
        local.append(pltpu.make_async_copy(w_src(a, z), w_dst(a, f), ls.at[a]))
        own = TG.at[a, blk(z, TB), blk(t, KB)]
        local.append(pltpu.make_async_copy(TK[a], own, ls.at[2 + a]))
    for d in local:
        d.start()
    pl.semaphore_wait(bar, FS - 1 + TP - 1)

    for a in range(2):
        send(w_src(a, z), w_dst(a, f), wx.at[a, z], DX)
    for q, (a, h) in enumerate(pieces):
        r = tgr(a, z, t, h)
        send(mine(a, h), r, ty.at[q, z], DY)
        send(mine(a, h), r, tc.at[q, z, y], DC)
    for i in range(1, Z):
        for a in range(2):
            send(w_src(a, order[i]), w_dst(a, f), wz.at[a, z], at_z(order[i]))
    up_z = jnp.minimum(z + 1, Z - 1)
    dn_z = jnp.maximum(z - 1, 0)
    for q, (a, h) in enumerate(pieces):
        r = tgr(a, z, t, h)
        send(mine(a, h), r, tz.at[q, z], at_z(up_z), z < Z - 1)
        send(mine(a, h), r, tz.at[q, z], at_z(dn_z), z > 0)

    def arrive(i, q):
        o = order[i]
        r = tgr(pieces[q][0], o, t, pieces[q][1])
        got(r, tz.at[q, o])
        send(r, r, tz.at[q, o], at_z(up_z), (o < z) & (z < Z - 1))
        send(r, r, tz.at[q, o], at_z(dn_z), (o > z) & (z > 0))
        send(r, r, ty.at[q, o], DY)
        send(r, r, tc.at[q, o, y], DC)

    def yfwd(i, q):
        o = order[i]
        r = tgr(pieces[q][0], o, yn * C + c, pieces[q][1])
        got(r, ty.at[q, o])
        send(r, r, tc.at[q, o, yn], DC)

    def ready(i):
        o = order[i]
        for q, (a, h) in enumerate(pieces):
            for yy in range(Y):
                got(tgr(a, o, yy * C + cn, h), tc.at[q, o, yy])

    def hidden(i):
        r = blk(order[i], TB)
        pre = dot(TG[0, r, :], UW[...], 1, 0)
        dact = dot(TG[1, r, :], DW[...], 1, 1)
        relued = jnp.maximum(pre, 0.0)
        ACT[r, :] = (relued * relued).astype(BF)
        DP[r, :] = (dact * 2.0 * relued).astype(BF)

    def back(i):
        o = order[i]
        d = DP[blk(o, TB), :]
        for yy in range(Y):
            for cc, keep in ((cn, False), (c, True)):
                part = dot(d, UW[blk(yy * C + cc, KB), :], 1, 1)
                if keep:
                    PO[o, yy] = part.astype(BF)
                else:
                    PCs[o, yy] = part.astype(BF)
                    send(PCs.at[o, yy], PCr.at[o, yy], pc.at[o, yy], DC)

    def core_sum(i):
        o = order[i]
        for yy in range(Y):
            got(PCr.at[o, yy], pc.at[o, yy])
        PYs[o] = (PO[o, yn].astype(F32) + PCr[o, yn].astype(F32)).astype(BF)
        send(PYs.at[o], PYr.at[o], py.at[o], DY)

    def from_z(side, o):
        got(PZr.at[side, o], pz.at[side, o])
        ACC[...] += PZr[side, o].astype(F32)

    def y_sum(o):
        ACC[...] = PO[o, y].astype(F32) + PCr[o, y].astype(F32) + PYr[o].astype(F32)

    def z_sum(o):
        got(PYr.at[o], py.at[o])
        y_sum(o)
        pl.when((o > z) & (z > 0))(lambda: from_z(0, o))
        pl.when((o < z) & (z < Z - 1))(lambda: from_z(1, o))
        PZs[o] = ACC[...].astype(BF)
        send(PZs.at[o], PZr.at[0, o], pz.at[0, o], at_z(up_z), o > z)
        send(PZs.at[o], PZr.at[1, o], pz.at[1, o], at_z(dn_z), o < z)

    def end_sum(o):
        got(PYr.at[o], py.at[o])
        y_sum(o)
        PZs[o] = ACC[...].astype(BF)
        send(PZs.at[o], PZd.at[z], pd.at[z], at_z(o), o != z)

    def from_end(zz):
        got(PZd.at[zz], pd.at[zz])
        ACC[...] += PZd[zz].astype(F32)

    def grads(a, ff):
        if a == 0:
            return dot(TG[0, :, blk(ff, RB)], DP[...], 0, 0)
        return dot(ACT[...], TG[1, :, blk(ff, RB)], 0, 0)

    for i in range(1, Z):
        o = order[i]
        for a in range(2):
            r = w_dst(a, o * X + x)
            got(r, wz.at[a, o])
            send(r, r, wx.at[a, o], DX)
    every = range(len(pieces))
    for q in every:
        yfwd(0, q)
    for q in every:
        arrive(1, q)
    for d in local:
        d.wait()
    for i in range(Z):
        for a in range(2):
            got(w_dst(a, order[i] * X + xn), wx.at[a, order[i]])
    for i in range(Z):
        ready(i)
        hidden(i)
        if i + 1 < Z:
            for q in every:
                yfwd(i + 1, q)
                if i + 2 < Z:
                    arrive(i + 2, q)
            if i + 2 == Z:
                for j in range(i):
                    core_sum(j)
            back(i)

    far = list(range(Z - 1, -1, -1))
    for i in far:
        for a in range(2):
            GXs[a, i] = grads(a, order[i] * X + xn).astype(BF)
            send(GXs.at[a, i], GXr.at[a, i], gx.at[a, i], DX)
    back(Z - 1)
    for i in range(max(Z - 2, 0), Z):
        core_sum(i)
    for j, i in enumerate(far):
        o = order[i]
        for a in range(2):
            g = grads(a, o * X + x)
            got(GXr.at[a, i], gx.at[a, i])
            g = g + GXr[a, i].astype(F32)
            if i:
                GZs[a, i] = g.astype(BF)
                send(GZs.at[a, i], GZr.at[a, z], gz.at[a, z], at_z(o))
            elif a == 0:
                ug_o[:, blk(o, HB)] = g
            else:
                dg_o[blk(o, HB), :] = g
        if j == 0:
            end_sum(jnp.int32(Z - 1))
            end_sum(jnp.int32(0))
    for o in range(1, Z - 1):
        z_sum(jnp.int32(o))
    y_sum(z)
    inner = (z > 0) & (z < Z - 1)
    pl.when(inner)(lambda: from_z(0, z))
    pl.when(inner)(lambda: from_z(1, z))
    for zz in range(Z):
        pl.when((z == 0) & (zz > 0) | (z == Z - 1) & (zz < Z - 1))(functools.partial(from_end, zz))
    ig_o[...] = ACC[...].astype(BF)

    for i in range(1, Z):
        o = order[i]
        for a in range(2):
            got(GZr.at[a, o], gz.at[a, o])
        ug_o[:, blk(o, HB)] = GZr[0, o].astype(F32)
        dg_o[blk(o, HB), :] = GZr[1, o].astype(F32)

    hi = dict(precision=lax.Precision.HIGHEST)
    g = ug_o[...]
    nu_mine = dot(jnp.ones((8, g.shape[1]), F32), g * g, 1, 1, **hi)
    NUs[...] = nu_mine
    for p in range(1, TP):
        send(NUs, NUr.at[t], nu.at[t], {"fs": f, "tp": (t + p) % TP})
    g = dg_o[...]
    nd_mine = dot(jnp.ones((8, g.shape[1]), F32), g * g, 1, 1, **hi)
    NDs[...] = nd_mine
    for p in range(1, FS):
        send(NDs, NDr.at[f], nd.at[f], {"fs": (f + p) % FS, "tp": t})
    NUr[t] = nu_mine
    NDr[f] = nd_mine
    for p in range(1, TP):
        q = (t + p) % TP
        got(NUr.at[q], nu.at[q])
    for p in range(1, FS):
        q = (f + p) % FS
        got(NDr.at[q], nd.at[q])
    un_o[...] = sum(NUr[q] for q in range(TP))[0:1, :]
    dn_o[...] = sum(NDr[q] for q in range(FS))[0:1, :]

    for d, cond in sends:
        if cond is None:
            d.wait_send()
        else:
            pl.when(cond)(d.wait_send)


def hand_over(*refs):
    n = len(refs) // 2
    copies = [pltpu.make_async_copy(refs[i], refs[n + i], refs[-1].at[i]) for i in range(n)]
    for d in copies:
        d.start()
    for d in copies:
        d.wait()


def fused(Z, tokens, grad_out, up_weight, down_weight):
    TB, KB = tokens.shape
    RB, HL = up_weight.shape
    HB, X, Y, C = HL // Z, 2, 2, 2
    FS, TP = Z * X, Y * C
    D, T = KB * TP, TB * Z
    V, S = pltpu.VMEM, pltpu.SemaphoreType.DMA
    any_ = pl.BlockSpec(memory_space=pl.ANY)
    vm = pl.BlockSpec(memory_space=pltpu.VMEM)
    H = 2
    n_sends = 48 * Z
    outs = pl.pallas_call(
        functools.partial(kernel, Z, H),
        out_shape=(
            jax.ShapeDtypeStruct((TB, KB), BF),
            jax.ShapeDtypeStruct((RB, HL), F32),
            jax.ShapeDtypeStruct((HL, RB), F32),
            jax.ShapeDtypeStruct((1, RB), F32),
            jax.ShapeDtypeStruct((1, HL), F32),
        ),
        in_specs=[any_] * 4,
        out_specs=[vm] * 5,
        scratch_shapes=[
            V((2, T, D), BF), V((D, HB), BF), V((HB, D), BF), V((T, HB), BF), V((T, HB), BF),
            V((Z, Y, TB, KB), BF), V((Z, Y, TB, KB), BF), V((Z, Y, TB, KB), BF),
            V((Z, TB, KB), BF), V((Z, TB, KB), BF), V((Z, TB, KB), BF), V((2, Z, TB, KB), BF), V((Z, TB, KB), BF), V((TB, KB), F32),
            V((2, Z, RB, HB), BF), V((2, Z, RB, HB), BF), V((2, Z, RB, HB), BF), V((2, Z, RB, HB), BF),
            V((8, RB), F32), V((TP, 8, RB), F32), V((8, HL), F32), V((FS, 8, HL), F32),
            S((n_sends,)), S((4,)), S((2, Z)), S((2, Z)), S((2 * H, Z)), S((2 * H, Z)), S((2 * H, Z, Y)),
            S((Z, Y)), S((Z,)), S((2, Z)), S((Z,)), S((2, Z)), S((2, Z)), S((TP,)), S((FS,)),
        ],
        compiler_params=pltpu.CompilerParams(
            collective_id=0, has_side_effects=True, vmem_limit_bytes=40 * 2**20
        ),
        name="ffn_bwd",
    )(tokens, grad_out, up_weight, down_weight)
    ig, ug, dg, un, dn = pl.pallas_call(
        hand_over,
        out_shape=tuple(jax.ShapeDtypeStruct(o.shape, o.dtype) for o in outs),
        in_specs=[vm] * 5,
        out_specs=[any_] * 5,
        scratch_shapes=[S((5,))],
        compiler_params=pltpu.CompilerParams(vmem_limit_bytes=8 * 2**20),
        name="hand_over",
    )(*outs)
    return ig, ug, dg, un.reshape(RB), dn.reshape(HL)


def solution(mesh):
    fs, tp = mesh.shape["fs"], mesh.shape["tp"]
    xs = tp // 2
    zs = fs // xs

    def body(tokens, grad_out, up_weight, down_weight):
        pairs = xs == 2 and tp == 4 and zs >= 2 and up_weight.shape[1] % (128 * zs) == 0
        fits = tokens.shape[0] * zs * tokens.shape[1] * tp * 4 <= 16 * 2**20
        square = up_weight.shape[0] == up_weight.shape[1] // zs
        if pairs and fits and square:
            return fused(zs, tokens, grad_out, up_weight, down_weight)
        return on_device(tokens, grad_out, up_weight, down_weight)

    return jax.shard_map(
        body,
        mesh=mesh,
        in_specs=(P("fs", "tp"), P("fs", "tp"), P("fs", "tp"), P("tp", "fs")),
        out_specs=(P("fs", "tp"), P("fs", "tp"), P("tp", "fs"), P("fs"), P("tp")),
        check_vma=False,
    )
```
